32 devices in a mesh: sp: 16 (over z, y, core), tp: 2 (over x).
Axes of the slice: x: 2, y: 2, z: 4, core: 2. Of those that a mesh axis runs over, the one named last changes fastest.
Arguments:
- activations: bfloat16 [4096, 2048], P('sp', 'tp'), may hold values from -8 to 8
- norm_gain: float32 [2048], replicated, may hold values from 0.1 to 1.9
- win_query: bfloat16 [2048, 1024], P(None, 'tp'), may hold values from -1 to 1
- win_key: bfloat16 [2048, 512], P(None, 'tp'), may hold values from -1 to 1
- win_value: bfloat16 [2048, 512], P(None, 'tp'), may hold values from -0.125 to 0.125
- sink_logit: float32 [16], P('tp'), may hold values from 1 to 6
- lat_query: bfloat16 [2048, 1536], P(None, 'tp'), may hold values from -1 to 1
- key_value_down_weight: bfloat16 [2048, 128], replicated, may hold values from -0.125 to 0.125
- rope_key: bfloat16 [2048, 64], replicated, may hold values from -1 to 1
- latent_norm_gain: float32 [128], replicated, may hold values from 0.1 to 1.9
- key_up_weight: bfloat16 [128, 1024], P(None, 'tp'), may hold values from -0.5 to 0.5
- value_up_weight: bfloat16 [128, 1024], P(None, 'tp'), may hold values from -0.5 to 0.5
- out_win: bfloat16 [1024, 2048], P('tp'), may hold values from -0.359375 to 0.359375
- out_lat: bfloat16 [1024, 2048], P('tp'), may hold values from -0.59765625 to 0.59765625
Outputs:
- mixed: bfloat16 [4096, 2048], P('sp', 'tp')
The draws below stay inside these ranges and needn't reach their ends.
All inputs are finite; a program needn't handle non-finite values.
Results may differ from the reference program's by a relative error of at most 0.025.
Values may be sent and summed in bfloat16 or wider, within the bound.
A program may use at most 64 MiB of HBM per device.

```python
import jax
import jax.numpy as jnp
from jax import lax

MODEL_WIDTH = 2048
HEADS_A = 16
KV_A = 8
DH = 64
WINDOW = 128
LATENT_HEADS = 8
LATENT_WIDTH = 128
UNROTATED_WIDTH = 128
D_ROPE = 64
VALUE_WIDTH = 128
TOK_DEV = 256
SEQ = 4096


def drawn(key, row_count, col_count, spread):
    values = jnp.clip(jax.random.normal(key, (row_count, col_count), jnp.float32) * spread, -1.0, 1.0)
    return values.astype(jnp.bfloat16)


def draw_activations(key, part):
    key_base = jax.random.fold_in(key, 11)
    values = jnp.clip(jax.random.normal(key_base, (SEQ, MODEL_WIDTH), jnp.float32), -6.0, 6.0)
    return values.astype(jnp.bfloat16)


def draw_win_query(key, part):
    return drawn(jax.random.fold_in(key, 21), MODEL_WIDTH, HEADS_A * DH, MODEL_WIDTH ** (-0.5))


def draw_win_key(key, part):
    return drawn(jax.random.fold_in(key, 22), MODEL_WIDTH, KV_A * DH, MODEL_WIDTH ** (-0.5))


def draw_lat_query(key, part):
    return drawn(jax.random.fold_in(key, 23), MODEL_WIDTH, LATENT_HEADS * (UNROTATED_WIDTH + D_ROPE), 2.5 * MODEL_WIDTH ** (-0.5))


def draw_rope_key(key, part):
    return drawn(jax.random.fold_in(key, 24), MODEL_WIDTH, D_ROPE, MODEL_WIDTH ** (-0.5))


def levels(stream_key, shape, split, least, largest):
    gain, own = 1.0, jax.random.fold_in(stream_key, 6)
    for position, shards_of in split:
        heights = jnp.exp(jax.random.uniform(jax.random.fold_in(own, position), (shards_of,), jnp.float32, least / len(split), largest / len(split)))
        gain = gain * jnp.repeat(heights, shape[position] // shards_of).reshape([-1 if axis == position else 1 for axis in range(len(shape))])
    return gain


def bell_draw(own_key, dims, scale, bound, shards=(), kind=jnp.bfloat16):
    result = jax.random.normal(own_key, dims, jnp.float32) * scale
    if len(shards) > 0:
        result = levels(own_key, dims, shards, -0.22, 0.18) * result
    return jnp.clip(result, min=-bound, max=bound).astype(kind)


def setup_inputs(seed: int = 0) -> dict:
    key_of = jax.random.split(jax.random.key(seed), 15)
    return {
        "activations": draw_activations(jax.random.fold_in(key_of[14], 71), 0),
        "norm_gain": jnp.clip(1.0 + 0.18 * jax.random.normal(key_of[1], (MODEL_WIDTH,), jnp.float32), 0.1, 1.9),
        "win_query": draw_win_query(jax.random.fold_in(key_of[14], 71), 0),
        "win_key": draw_win_key(jax.random.fold_in(key_of[14], 71), 0),
        "win_value": bell_draw(key_of[4], (MODEL_WIDTH, KV_A * DH), MODEL_WIDTH ** -0.5, 0.125, ((1, 2),)),
        "sink_logit": jnp.clip(1.0 + 5.0 * jax.random.uniform(key_of[5], (HEADS_A,), jnp.float32) ** levels(key_of[5], (HEADS_A,), ((0, 2),), -0.2, 0.2), 1.0, 6.0),
        "lat_query": draw_lat_query(jax.random.fold_in(key_of[14], 71), 0),
        "key_value_down_weight": bell_draw(key_of[7], (MODEL_WIDTH, LATENT_WIDTH), MODEL_WIDTH ** -0.5, 0.125),
        "rope_key": draw_rope_key(jax.random.fold_in(key_of[14], 71), 0),
        "latent_norm_gain": jnp.clip(1.0 + 0.18 * jax.random.normal(key_of[9], (LATENT_WIDTH,), jnp.float32), 0.1, 1.9),
        "key_up_weight": bell_draw(key_of[10], (LATENT_WIDTH, LATENT_HEADS * UNROTATED_WIDTH), LATENT_WIDTH ** -0.5, 0.5, ((1, 2),)),
        "value_up_weight": bell_draw(key_of[11], (LATENT_WIDTH, LATENT_HEADS * VALUE_WIDTH), LATENT_WIDTH ** -0.5, 0.5, ((1, 2),)),
        "out_win": bell_draw(key_of[12], (HEADS_A * DH, MODEL_WIDTH), 0.06, 0.359375, ((0, 2),)),
        "out_lat": bell_draw(key_of[13], (LATENT_HEADS * VALUE_WIDTH, MODEL_WIDTH), 0.1, 0.59765625, ((0, 2),)),
    }


EPSILON = 1e-06
ROPE_BASE = 10000.0

def rotate(vectors, angles):
    half_width = vectors.shape[-1] // 2
    cosine_table = jnp.cos(angles)
    sine_table = jnp.sin(angles)
    lower_half = vectors[..., :half_width]
    upper_half = vectors[..., half_width:]
    return jnp.concatenate([lower_half * cosine_table - upper_half * sine_table, lower_half * sine_table + upper_half * cosine_table], axis=-1)

def rotary_angles(places, width):
    frequency = 1.0 / ROPE_BASE ** (jnp.arange(0, width, 2).astype(jnp.float32) / width)
    return places[:, None] * frequency[None, :]

def reference(activations, norm_gain, win_query, win_key, win_value, sink_logit, lat_query, key_value_down_weight, rope_key, latent_norm_gain, key_up_weight, value_up_weight, out_win, out_lat):
    widened = activations.astype(jnp.float32)
    row_scale = lax.rsqrt(lax.optimization_barrier(jnp.mean(widened * widened, axis=1)) + EPSILON)[:, None]
    normalized = (widened * norm_gain[None, :]).astype(jnp.bfloat16)

    def project(weight):
        return jnp.dot(normalized, weight, preferred_element_type=jnp.float32)
    win_queries = (project(win_query) * row_scale).astype(jnp.bfloat16)
    win_keys = (project(win_key) * row_scale).astype(jnp.bfloat16)
    win_values = (project(win_value) * row_scale).astype(jnp.bfloat16)
    places = jnp.arange(SEQ).astype(jnp.float32)
    angles = rotary_angles(places, D_ROPE)
    query_all = (project(lat_query) * row_scale).reshape(SEQ, LATENT_HEADS, UNROTATED_WIDTH + D_ROPE)
    query_plain = query_all[..., :UNROTATED_WIDTH].astype(jnp.bfloat16)
    query_turned = rotate(query_all[..., UNROTATED_WIDTH:], angles[:, None, :]).astype(jnp.bfloat16)
    compressed = project(key_value_down_weight)
    latent = (compressed * lax.rsqrt(lax.optimization_barrier(jnp.mean(compressed * compressed, axis=1, keepdims=True)) + EPSILON) * latent_norm_gain[None, :]).astype(jnp.bfloat16)
    key_rotary = rotate(project(rope_key) * row_scale, angles).astype(jnp.bfloat16)
    key_nope = jnp.dot(latent, key_up_weight, preferred_element_type=jnp.float32).astype(jnp.bfloat16)
    value_lat = jnp.dot(latent, value_up_weight, preferred_element_type=jnp.float32).astype(jnp.bfloat16)
    block_count = SEQ // WINDOW
    groups = HEADS_A // KV_A
    query_blocks = win_queries.reshape(block_count, WINDOW, KV_A, groups, DH)
    zero_rim = jnp.zeros((WINDOW, KV_A * DH), jnp.bfloat16)
    key_padded = jnp.concatenate([zero_rim, win_keys, zero_rim], 0).reshape(block_count + 2, WINDOW, KV_A, DH)
    value_padded = jnp.concatenate([zero_rim, win_values, zero_rim], 0).reshape(block_count + 2, WINDOW, KV_A, DH)
    key_near = jnp.concatenate([key_padded[:-2], key_padded[1:-1], key_padded[2:]], axis=1)
    value_near = jnp.concatenate([value_padded[:-2], value_padded[1:-1], value_padded[2:]], axis=1)
    slopes = jnp.exp2(-8.0 * jnp.arange(1, HEADS_A + 1).astype(jnp.float32) / HEADS_A).reshape(KV_A, groups)
    sink_table = sink_logit.reshape(KV_A, groups)

    def window_block(inputs):
        query_block, key_block, value_block, block_index = inputs
        query_pos = block_index * WINDOW + jnp.arange(WINDOW, dtype=jnp.int32)
        key_pos = (block_index - 1) * WINDOW + jnp.arange(3 * WINDOW, dtype=jnp.int32)
        distance = jnp.abs(query_pos[:, None] - key_pos[None, :])
        in_window = (distance <= WINDOW) & (key_pos[None, :] >= 0) & (key_pos[None, :] < SEQ)
        scores = jnp.einsum('qhgd,khd->hgqk', query_block.astype(jnp.float32), key_block.astype(jnp.float32)) * DH ** (-0.5)
        scores = scores - slopes[:, :, None, None] * distance.astype(jnp.float32)[None, None]
        scores = jnp.where(in_window[None, None], scores, -jnp.inf)
        row_peak = jnp.maximum(lax.optimization_barrier(jnp.max(scores, axis=3)), sink_table[:, :, None])
        weights = jnp.exp(scores - row_peak[..., None])
        denominator = lax.optimization_barrier(jnp.sum(weights, axis=3)) + jnp.exp(sink_table[:, :, None] - row_peak)
        rounded = lax.optimization_barrier(weights.astype(jnp.bfloat16)).astype(jnp.float32)
        blended = jnp.einsum('hgqk,khd->qhgd', rounded, value_block.astype(jnp.float32))
        blended = blended / jnp.transpose(denominator, (2, 0, 1))[..., None]
        return blended.reshape(WINDOW, HEADS_A * DH).astype(jnp.bfloat16)
    win_out = lax.map(window_block, (query_blocks, key_near, value_near, jnp.arange(block_count, dtype=jnp.int32))).reshape(SEQ, HEADS_A * DH)
    span_count = SEQ // TOK_DEV
    plain_keys = key_nope.astype(jnp.float32).reshape(SEQ, LATENT_HEADS, UNROTATED_WIDTH)
    lat_values = value_lat.astype(jnp.float32).reshape(SEQ, LATENT_HEADS, VALUE_WIDTH)
    turned_keys = key_rotary.astype(jnp.float32)

    def latent_block(inputs):
        plain_block, turned_block = inputs
        scores = (jnp.einsum('qhd,khd->hqk', plain_block.astype(jnp.float32), plain_keys) + jnp.einsum('qhd,kd->hqk', turned_block.astype(jnp.float32), turned_keys)) * (UNROTATED_WIDTH + D_ROPE) ** (-0.5)
        row_peak = lax.optimization_barrier(jnp.max(scores, axis=2, keepdims=True))
        weights = jnp.exp(scores - row_peak)
        totals = lax.optimization_barrier(jnp.sum(weights, axis=2))
        rounded = lax.optimization_barrier(weights.astype(jnp.bfloat16)).astype(jnp.float32)
        blended = jnp.einsum('hqk,khd->qhd', rounded, lat_values) / jnp.transpose(totals)[..., None]
        return blended.reshape(TOK_DEV, LATENT_HEADS * VALUE_WIDTH).astype(jnp.bfloat16)
    lat_out = lax.map(latent_block, (query_plain.reshape(span_count, TOK_DEV, LATENT_HEADS, UNROTATED_WIDTH), query_turned.reshape(span_count, TOK_DEV, LATENT_HEADS, D_ROPE))).reshape(SEQ, LATENT_HEADS * VALUE_WIDTH)
    summed = jnp.dot(win_out, out_win, preferred_element_type=jnp.float32) + jnp.dot(lat_out, out_lat, preferred_element_type=jnp.float32)
    return summed.astype(jnp.bfloat16)
```

```python
import functools

import jax
import jax.numpy as jnp
import numpy as np
from jax import lax
from jax.experimental import pallas as pl
from jax.experimental.pallas import tpu as pltpu
from jax.sharding import PartitionSpec as P

HEADS_A = 16
DH = 64
WINDOW = 128
UNROTATED_WIDTH = 128
D_ROPE = 64
VALUE_WIDTH = 128

EPSILON = 1e-06
ROPE_BASE = 10000.0
LOG2E = 1.4426950408889634
MESH = pl.DeviceIdType.MESH
F32 = jnp.float32
BF16 = jnp.bfloat16
SUB = 2


def turn(vectors, cosine, sine):
    half = vectors.shape[-1] // 2
    swapped = jnp.concatenate([vectors[:, half:], vectors[:, :half]], axis=1)
    return vectors * cosine + swapped * sine


def dot_nt(a, b):
    return lax.dot_general(a, b, (((1,), (1,)), ((), ())), preferred_element_type=F32)


def project_kernel(
    n_sp, n_tp,
    x_ref, gain_ref, cos_ref, sin_ref, sink_ref, slope_ref, lng_ref, kup_ref,
    wkv_hbm, wr_hbm, wk_hbm, wv_hbm, wq_hbm, wlq_hbm,
    q_ref, kv_ref, win_ref,
    x_all, wkv, wr, wk, wv, wq, wlq, akv, ar, ak, av, aq, alq, sq, gath, halo, qwin,
    w_sem, x_send, x_recv, z_send, z_recv, y_send, y_recv, c_send, c_recv, h_send, h_recv,
):
    sp = lax.axis_index("sp")
    tp = lax.axis_index("tp")
    rows, local = x_ref.shape
    part = local // SUB
    hi = n_sp // 4
    z, y, c = sp // 4, (sp // 2) % 2, sp % 2

    def at(zz, yy, cc):
        return (zz * 2 + yy) * 2 + cc

    right, left = (sp + 1) % n_sp, (sp + n_sp - 1) % n_sp

    weights = ((wkv_hbm, wkv), (wr_hbm, wr), (wk_hbm, wk), (wv_hbm, wv), (wq_hbm, wq), (wlq_hbm, wlq))
    loads = [pltpu.make_async_copy(a, b, w_sem.at[i]) for i, (a, b) in enumerate(weights)]
    for load in loads:
        load.start()

    barrier = pltpu.get_barrier_semaphore()
    peers = [(sp, (tp + s) % n_tp) for s in range(1, n_tp)]
    peers += [(at((z + d) % hi, y, c), tp) for d in range(1, hi)]
    peers += [(at(z, 1 - y, c), tp), (at(z, y, 1 - c), tp), (right, tp), (left, tp)]
    for peer in peers:
        pl.semaphore_signal(barrier, inc=1, device_id=peer, device_id_type=MESH)
    pl.semaphore_wait(barrier, len(peers))

    def remote(src, dst, send, recv, device):
        return pltpu.make_async_remote_copy(
            src_ref=src, dst_ref=dst, send_sem=send, recv_sem=recv, device_id=device, device_id_type=MESH
        )

    x_copies = {}
    for cc in range(SUB):
        for s in range(1, n_tp):
            x_copies[s, cc] = remote(
                x_ref.at[:, cc * part : (cc + 1) * part],
                x_all.at[tp * SUB + cc],
                x_send.at[s, cc],
                x_recv.at[s, cc],
                (sp, (tp + s) % n_tp),
            )
            x_copies[s, cc].start()

    def add_in(block, slot, pairs, first):
        where = pl.ds(pl.multiple_of(slot * part, part), part)
        for weight, acc in pairs:
            term = jnp.dot(block, weight[where, :], preferred_element_type=F32)
            acc[...] = term if first else acc[...] + term

    def norm_block(raw, slot, first):
        wide = raw.astype(F32)
        total = jnp.broadcast_to(jnp.sum(wide * wide, axis=1, keepdims=True), sq.shape)
        sq[...] = total if first else sq[...] + total
        return (wide * gain_ref[slot]).astype(BF16)

    small = ((wkv, akv), (wr, ar))
    big = ((wk, ak), (wv, av), (wq, aq), (wlq, alq))
    for load in loads:
        load.wait()
    for cc in range(SUB):
        slot = tp * SUB + cc
        block = norm_block(x_ref[:, cc * part : (cc + 1) * part], slot, cc == 0)
        add_in(block, slot, small + big, cc == 0)
    steps = [(s, cc) for cc in range(SUB) for s in range(1, n_tp)]
    for s, cc in steps[:-1]:
        x_copies[s, cc].wait_recv()
        slot = ((tp + n_tp - s) % n_tp) * SUB + cc
        add_in(norm_block(x_all[slot], slot, False), slot, small + big, False)
    s, cc = steps[-1]
    x_copies[s, cc].wait_recv()
    last_slot = ((tp + n_tp - s) % n_tp) * SUB + cc
    last_block = norm_block(x_all[last_slot], last_slot, False)
    add_in(last_block, last_slot, small, False)

    scale = lax.rsqrt(sq[:, 0:1] / (local * n_tp) + EPSILON)
    comp = akv[...]
    latent = comp * lax.rsqrt(jnp.mean(comp * comp, axis=1, keepdims=True) + EPSILON) * lng_ref[...]
    rotary = turn(ar[...] * scale, cos_ref[...], sin_ref[...])
    gath[sp, 0:rows, :] = latent.astype(BF16)
    gath[sp, rows : rows + rows // 2, :] = jnp.concatenate(
        [rotary[: rows // 2], rotary[rows // 2 :]], axis=1
    ).astype(BF16)

    def forward(block, sends, recvs, index, device):
        copy = remote(gath.at[block], gath.at[block], sends.at[index], recvs.at[index], device)
        copy.start()
        return copy

    to_y, to_c = (at(z, 1 - y, c), tp), (at(z, y, 1 - c), tp)
    z_copies = [forward(sp, z_send, z_recv, d, (at((z + d) % hi, y, c), tp)) for d in range(1, hi)]
    y_copies = [forward(sp, y_send, y_recv, 0, to_y)]
    c_copies = [forward(sp, c_send, c_recv, 0, to_c)]

    add_in(last_block, last_slot, big, False)
    k_cols = ak.shape[1]
    halo[WINDOW : WINDOW + rows, 0:k_cols] = (ak[...] * scale).astype(BF16)
    halo[WINDOW : WINDOW + rows, k_cols : 2 * k_cols] = (av[...] * scale).astype(BF16)
    h_copies = [
        remote(halo.at[rows : rows + WINDOW], halo.at[0:WINDOW], h_send.at[0], h_recv.at[0], (right, tp)),
        remote(
            halo.at[WINDOW : 2 * WINDOW],
            halo.at[rows + WINDOW : rows + 2 * WINDOW],
            h_send.at[1],
            h_recv.at[1],
            (left, tp),
        ),
    ]
    for copy in h_copies:
        copy.start()
    qwin[...] = (aq[...] * scale).astype(BF16)
    per_head = UNROTATED_WIDTH + D_ROPE
    factor = per_head ** (-0.5) * LOG2E
    for h in range(alq.shape[1] // per_head):
        one = alq[:, h * per_head : (h + 1) * per_head] * scale
        plain = one[:, :UNROTATED_WIDTH].astype(BF16)
        seen = dot_nt(plain, kup_ref[:, h * UNROTATED_WIDTH : (h + 1) * UNROTATED_WIDTH]) * factor
        turned = turn(one[:, UNROTATED_WIDTH:], cos_ref[...], sin_ref[...]) * factor
        q_ref[h, :, 0:UNROTATED_WIDTH] = seen.astype(BF16)
        q_ref[h, :, UNROTATED_WIDTH:] = jnp.concatenate([turned, jnp.zeros_like(turned)], axis=1).astype(BF16)

    for d in range(1, hi):
        z_copies[d - 1].wait_recv()
        block = at((z + hi - d) % hi, y, c)
        y_copies.append(forward(block, y_send, y_recv, d, to_y))
        c_copies.append(forward(block, c_send, c_recv, d, to_c))
    for copy in h_copies:
        copy.wait()

    span = 3 * WINDOW
    spots = lax.broadcasted_iota(jnp.int32, (WINDOW, span), 0)
    keys_at = lax.broadcasted_iota(jnp.int32, (WINDOW, span), 1)
    distance = jnp.abs(spots + WINDOW - keys_at)
    far = distance.astype(F32)
    seq_total = rows * n_sp

    def window(kv_head):
        for b in range(rows // WINDOW):
            key_pos = sp * rows + (b - 1) * WINDOW + keys_at
            inside = (distance <= WINDOW) & (key_pos >= 0) & (key_pos < seq_total)
            keys = halo[b * WINDOW : b * WINDOW + span, kv_head * DH : (kv_head + 1) * DH]
            values = halo[b * WINDOW : b * WINDOW + span, k_cols + kv_head * DH : k_cols + (kv_head + 1) * DH]
            pieces = []
            for g in range(2):
                head = kv_head * 2 + g
                query = qwin[b * WINDOW : (b + 1) * WINDOW, head * DH : (head + 1) * DH]
                scores = dot_nt(query, keys) * DH ** (-0.5) - slope_ref[head] * far
                scores = jnp.where(inside, scores, -jnp.inf)
                peak = jnp.maximum(jnp.max(scores, axis=1, keepdims=True), sink_ref[head])
                weight = jnp.exp(scores - peak)
                bottom = jnp.sum(weight, axis=1, keepdims=True) + jnp.exp(sink_ref[head] - peak)
                blended = jnp.dot(weight.astype(BF16), values, preferred_element_type=F32)
                pieces.append(blended / bottom)
            win_ref[b * WINDOW : (b + 1) * WINDOW, kv_head * 2 * DH : (kv_head + 1) * 2 * DH] = (
                jnp.concatenate(pieces, axis=1).astype(BF16)
            )

    kv_heads = k_cols // DH
    for kv_head in range((kv_heads + 1) // 2):
        window(kv_head)
    for d in range(hi):
        y_copies[d].wait_recv()
        c_copies.append(forward(at((z + hi - d) % hi, 1 - y, c), c_send, c_recv, hi + d, to_c))
    for kv_head in range((kv_heads + 1) // 2, kv_heads):
        window(kv_head)

    lanes = lax.broadcasted_iota(jnp.int32, (rows // 2, D_ROPE), 1)
    mark = jnp.where(lanes == 0, 1.0, 0.0).astype(BF16)

    def assemble(block):
        base = pl.multiple_of(block * rows, rows)
        kv_ref[pl.ds(base, rows), 0:UNROTATED_WIDTH] = gath[block, 0:rows, :]
        both = gath[block, rows : rows + rows // 2, :]
        kv_ref[pl.ds(base, rows // 2), UNROTATED_WIDTH:] = jnp.concatenate([both[:, :D_ROPE], mark], axis=1)
        kv_ref[pl.ds(base + rows // 2, rows // 2), UNROTATED_WIDTH:] = jnp.concatenate(
            [both[:, D_ROPE:], mark], axis=1
        )

    for d in range(hi):
        assemble(at((z + hi - d) % hi, y, c))
        assemble(at((z + hi - d) % hi, 1 - y, c))
    for d in range(hi):
        c_copies[d].wait_recv()
        assemble(at((z + hi - d) % hi, y, 1 - c))
    for d in range(hi):
        c_copies[hi + d].wait_recv()
        assemble(at((z + hi - d) % hi, 1 - y, 1 - c))
    for copy in list(x_copies.values()) + z_copies + y_copies + c_copies:
        copy.wait_send()


def attend_kernel(
    n_tp,
    q_ref, kv_ref, win_ref, vup_ref, ow_hbm, ol_hbm,
    out_ref,
    ow, ol, acc, peak, lat, outgoing, incoming, own, w_sem, send, recv,
):
    sp = lax.axis_index("sp")
    tp = lax.axis_index("tp")
    heads, rows, _ = q_ref.shape
    half = rows // 2
    cols = out_ref.shape[1]
    loads = [pltpu.make_async_copy(ow_hbm, ow, w_sem.at[0]), pltpu.make_async_copy(ol_hbm, ol, w_sem.at[1])]
    for load in loads:
        load.start()
    barrier = pltpu.get_barrier_semaphore()
    for s in range(1, n_tp):
        pl.semaphore_signal(barrier, inc=1, device_id=(sp, (tp + s) % n_tp), device_id_type=MESH)
    pl.semaphore_wait(barrier, n_tp - 1)

    chunk = min(1024, kv_ref.shape[0])
    copies = []
    for b in range(2):
        query = jnp.concatenate([q_ref[h, b * half : (b + 1) * half, :] for h in range(heads)], axis=0)
        acc[...] = jnp.zeros_like(acc)
        peak[...] = jnp.full_like(peak, -jnp.inf)

        def step(i, carry):
            keys = kv_ref[pl.ds(pl.multiple_of(i * chunk, chunk), chunk), :]
            scores = dot_nt(query, keys)
            old = peak[:, 0:1]
            new = jnp.maximum(old, jnp.max(scores, axis=1, keepdims=True))
            weight = jnp.exp2(scores - new).astype(BF16)
            acc[...] = acc[...] * jnp.exp2(old - new) + jnp.dot(weight, keys, preferred_element_type=F32)
            peak[...] = jnp.broadcast_to(new, peak.shape)
            return carry

        lax.fori_loop(0, kv_ref.shape[0] // chunk, step, 0)
        bottom = acc[:, UNROTATED_WIDTH + D_ROPE : UNROTATED_WIDTH + D_ROPE + 1]
        blended = (acc[:, 0:VALUE_WIDTH] / bottom).astype(BF16)
        for h in range(heads):
            where = slice(h * VALUE_WIDTH, (h + 1) * VALUE_WIDTH)
            lat[:, where] = jnp.dot(
                blended[h * half : (h + 1) * half], vup_ref[:, where], preferred_element_type=F32
            ).astype(BF16)
        if b == 0:
            for load in loads:
                load.wait()
        won = win_ref[b * half : (b + 1) * half, :]

        def terms(j):
            where = pl.ds(pl.multiple_of(j * cols, cols), cols)
            return jnp.dot(won, ow[:, where], preferred_element_type=F32) + jnp.dot(
                lat[...], ol[:, where], preferred_element_type=F32
            )

        for s in range(1, n_tp):
            other = (tp + s) % n_tp
            outgoing[b, s - 1] = terms(other).astype(BF16)
            copy = pltpu.make_async_remote_copy(
                src_ref=outgoing.at[b, s - 1],
                dst_ref=incoming.at[b, s - 1],
                send_sem=send.at[b, s],
                recv_sem=recv.at[b, s],
                device_id=(sp, other),
                device_id_type=MESH,
            )
            copy.start()
            copies.append((b, s, copy))
        own[b] = terms(tp)
    for b in range(2):
        total = own[b]
        for bb, s, copy in copies:
            if bb == b:
                copy.wait()
                total = total + incoming[b, s - 1].astype(F32)
        out_ref[b * half : (b + 1) * half, :] = total.astype(BF16)


def per_device(
    n_sp, n_tp,
    activations, norm_gain, win_query, win_key, win_value, sink_logit, lat_query,
    key_value_down_weight, rope_key, latent_norm_gain, key_up_weight, value_up_weight, out_win, out_lat,
):
    rows, local = activations.shape
    width = local * n_tp
    part = local // SUB
    heads_a = sink_logit.shape[0]
    heads_l = lat_query.shape[1] // (UNROTATED_WIDTH + D_ROPE)
    places = (lax.axis_index("sp") * rows + jnp.arange(rows, dtype=jnp.int32)).astype(F32)
    frequency = 1.0 / ROPE_BASE ** (jnp.arange(0, D_ROPE, 2).astype(F32) / D_ROPE)
    angles = places[:, None] * frequency[None, :]
    cosine, sine = jnp.cos(angles), jnp.sin(angles)
    cosine = jnp.concatenate([cosine, cosine], axis=1)
    sine = jnp.concatenate([-sine, sine], axis=1)
    head_ids = lax.axis_index("tp") * heads_a + jnp.arange(heads_a, dtype=jnp.int32)
    slopes = jnp.exp2(-8.0 * (head_ids + 1).astype(F32) / HEADS_A)

    vmem = pl.BlockSpec(memory_space=pltpu.VMEM)
    smem = pl.BlockSpec(memory_space=pltpu.SMEM)
    hbm = pl.BlockSpec(memory_space=pl.ANY)
    weights = (key_value_down_weight, rope_key, win_key, win_value, win_query, lat_query)
    hi = n_sp // 4
    dma = pltpu.SemaphoreType.DMA
    packed = rows + rows // 2
    query, keys, win_out = pl.pallas_call(
        functools.partial(project_kernel, n_sp, n_tp),
        out_shape=(
            jax.ShapeDtypeStruct((heads_l, rows, 2 * UNROTATED_WIDTH), BF16),
            jax.ShapeDtypeStruct((rows * n_sp, 2 * UNROTATED_WIDTH), BF16),
            jax.ShapeDtypeStruct((rows, heads_a * DH), BF16),
        ),
        in_specs=[vmem, vmem, vmem, vmem, smem, smem, vmem, vmem] + [hbm] * 6,
        out_specs=(vmem, vmem, vmem),
        scratch_shapes=[pltpu.VMEM((n_tp * SUB, rows, part), BF16)]
        + [pltpu.VMEM(w.shape, BF16) for w in weights]
        + [pltpu.VMEM((rows, w.shape[1]), F32) for w in weights]
        + [
            pltpu.VMEM((rows, 128), F32),
            pltpu.VMEM((n_sp, packed, UNROTATED_WIDTH), BF16),
            pltpu.VMEM((rows + 2 * WINDOW, 2 * win_key.shape[1]), BF16),
            pltpu.VMEM((rows, win_query.shape[1]), BF16),
            dma((6,)),
            dma((n_tp, SUB)), dma((n_tp, SUB)),
            dma((hi,)), dma((hi,)),
            dma((hi,)), dma((hi,)),
            dma((2 * hi,)), dma((2 * hi,)),
            dma((2,)), dma((2,)),
        ],
        compiler_params=pltpu.CompilerParams(
            collective_id=0, has_side_effects=True, vmem_limit_bytes=56 * 1024 * 1024
        ),
        name="project",
    )(
        activations, norm_gain.reshape(n_tp * SUB, 1, part), cosine, sine, sink_logit, slopes,
        latent_norm_gain.reshape(1, -1), key_up_weight, *weights,
    )
    return pl.pallas_call(
        functools.partial(attend_kernel, n_tp),
        out_shape=jax.ShapeDtypeStruct((rows, width // n_tp), BF16),
        in_specs=[vmem, vmem, vmem, vmem, hbm, hbm],
        out_specs=vmem,
        scratch_shapes=[
            pltpu.VMEM(out_win.shape, BF16),
            pltpu.VMEM(out_lat.shape, BF16),
            pltpu.VMEM((heads_l * rows // 2, 2 * UNROTATED_WIDTH), F32),
            pltpu.VMEM((heads_l * rows // 2, 128), F32),
            pltpu.VMEM((rows // 2, heads_l * VALUE_WIDTH), BF16),
            pltpu.VMEM((2, n_tp - 1, rows // 2, width // n_tp), BF16),
            pltpu.VMEM((2, n_tp - 1, rows // 2, width // n_tp), BF16),
            pltpu.VMEM((2, rows // 2, width // n_tp), F32),
            dma((2,)),
            dma((2, n_tp)), dma((2, n_tp)),
        ],
        compiler_params=pltpu.CompilerParams(
            collective_id=1, has_side_effects=True, vmem_limit_bytes=56 * 1024 * 1024
        ),
        name="attend",
    )(query, keys, win_out, value_up_weight, out_win, out_lat)


def solution(mesh):
    return jax.shard_map(
        functools.partial(per_device, mesh.shape["sp"], mesh.shape["tp"]),
        mesh=mesh,
        in_specs=(
            P("sp", "tp"),
            P(),
            P(None, "tp"),
            P(None, "tp"),
            P(None, "tp"),
            P("tp"),
            P(None, "tp"),
            P(),
            P(),
            P(),
            P(None, "tp"),
            P(None, "tp"),
            P("tp", None),
            P("tp", None),
        ),
        out_specs=P("sp", "tp"),
        check_vma=False,
    )
```

```python
import functools

import jax
import jax.numpy as jnp
import numpy as np
from jax import lax
from jax.experimental import pallas as pl
from jax.experimental.pallas import tpu as pltpu
from jax.sharding import PartitionSpec as P

HEADS_A = 16
DH = 64
WINDOW = 128
UNROTATED_WIDTH = 128
D_ROPE = 64
VALUE_WIDTH = 128

EPSILON = 1e-06
ROPE_BASE = 10000.0
LOG2E = 1.4426950408889634
MESH = pl.DeviceIdType.MESH
F32 = jnp.float32
BF16 = jnp.bfloat16
SUB = 2


def turn(vectors, cosine, sine):
    half = vectors.shape[-1] // 2
    swapped = jnp.concatenate([vectors[:, half:], vectors[:, :half]], axis=1)
    return vectors * cosine + swapped * sine


def dot_nt(a, b):
    return lax.dot_general(a, b, (((1,), (1,)), ((), ())), preferred_element_type=F32)


def project_kernel(
    n_sp, n_tp,
    x_ref, gain_ref, near_ref, base_ref, sink_ref, lng_ref, kup_ref,
    wkv_hbm, wr_hbm, wk_hbm, wv_hbm, wq_hbm, wlq_hbm,
    q_ref, kv_ref, win_ref,
    x_all, wkv, wr, wk, wv, wq, wlq, akv, ar, ak, av, aq, alq, sq, gath, halo, qwin,
    w_sem, x_send, x_recv, z_send, z_recv, y_send, y_recv, c_send, c_recv, h_send, h_recv,
):
    sp = lax.axis_index("sp")
    tp = lax.axis_index("tp")
    rows, local = x_ref.shape
    part = local // SUB
    hi = n_sp // 4
    z, y, c = sp // 4, (sp // 2) % 2, sp % 2

    def at(zz, yy, cc):
        return (zz * 2 + yy) * 2 + cc

    right, left = (sp + 1) % n_sp, (sp + n_sp - 1) % n_sp

    weights = ((wkv_hbm, wkv), (wr_hbm, wr), (wk_hbm, wk), (wv_hbm, wv), (wq_hbm, wq), (wlq_hbm, wlq))
    loads = [pltpu.make_async_copy(a, b, w_sem.at[i]) for i, (a, b) in enumerate(weights)]
    for load in loads:
        load.start()

    barrier = pltpu.get_barrier_semaphore()
    peers = [(sp, (tp + s) % n_tp) for s in range(1, n_tp)]
    peers += [(at((z + d) % hi, y, c), tp) for d in range(1, hi)]
    peers += [(at(z, 1 - y, c), tp), (at(z, y, 1 - c), tp), (right, tp), (left, tp)]
    for peer in peers:
        pl.semaphore_signal(barrier, inc=1, device_id=peer, device_id_type=MESH)
    pl.semaphore_wait(barrier, len(peers))

    def remote(src, dst, send, recv, device):
        return pltpu.make_async_remote_copy(
            src_ref=src, dst_ref=dst, send_sem=send, recv_sem=recv, device_id=device, device_id_type=MESH
        )

    x_copies = {}
    for cc in range(SUB):
        for s in range(1, n_tp):
            x_copies[s, cc] = remote(
                x_ref.at[:, cc * part : (cc + 1) * part],
                x_all.at[tp * SUB + cc],
                x_send.at[s, cc],
                x_recv.at[s, cc],
                (sp, (tp + s) % n_tp),
            )
            x_copies[s, cc].start()

    def add_in(block, slot, pairs, first):
        where = pl.ds(pl.multiple_of(slot * part, part), part)
        for weight, acc in pairs:
            if weight is wr:
                term = dot_nt(block, weight[:, where])
            else:
                term = jnp.dot(block, weight[where, :], preferred_element_type=F32)
            acc[...] = term if first else acc[...] + term

    def norm_block(raw, slot, first):
        wide = raw.astype(F32)
        total = jnp.broadcast_to(jnp.sum(wide * wide, axis=1, keepdims=True), sq.shape)
        sq[...] = total if first else sq[...] + total
        return (wide * gain_ref[slot]).astype(BF16)

    near_cos, near_sin = near_ref[0], near_ref[1]
    base_cos, base_sin = base_ref[sp, 0:1, :], base_ref[sp, 1:2, :]
    cosine = near_cos * base_cos - near_sin * base_sin
    plain_sine = near_sin * base_cos + near_cos * base_sin
    lane = lax.broadcasted_iota(jnp.int32, plain_sine.shape, 1)
    sine = jnp.where(lane < D_ROPE // 2, -plain_sine, plain_sine)
    small = ((wkv, akv), (wr, ar))
    big = ((wk, ak), (wv, av), (wq, aq), (wlq, alq))
    for load in loads:
        load.wait()
    for cc in range(SUB):
        slot = tp * SUB + cc
        block = norm_block(x_ref[:, cc * part : (cc + 1) * part], slot, cc == 0)
        add_in(block, slot, small + big, cc == 0)
    steps = [(s, cc) for cc in range(SUB) for s in range(1, n_tp)]
    for s, cc in steps[:-1]:
        x_copies[s, cc].wait_recv()
        slot = ((tp + n_tp - s) % n_tp) * SUB + cc
        add_in(norm_block(x_all[slot], slot, False), slot, small + big, False)
    s, cc = steps[-1]
    x_copies[s, cc].wait_recv()
    last_slot = ((tp + n_tp - s) % n_tp) * SUB + cc
    last_block = norm_block(x_all[last_slot], last_slot, False)
    add_in(last_block, last_slot, small, False)

    scale = lax.rsqrt(sq[:, 0:1] / (local * n_tp) + EPSILON)
    comp = akv[...]
    latent = comp * lax.rsqrt(jnp.mean(comp * comp, axis=1, keepdims=True) + EPSILON) * lng_ref[...]
    rotary = turn(ar[...] * scale, cosine, sine)
    gath[sp, 0:rows, :] = latent.astype(BF16)
    gath[sp, rows : rows + rows // 2, :] = jnp.concatenate(
        [rotary[: rows // 2], rotary[rows // 2 :]], axis=1
    ).astype(BF16)

    def forward(block, sends, recvs, index, device):
        copy = remote(gath.at[block], gath.at[block], sends.at[index], recvs.at[index], device)
        copy.start()
        return copy

    to_y, to_c = (at(z, 1 - y, c), tp), (at(z, y, 1 - c), tp)
    z_copies = [forward(sp, z_send, z_recv, d, (at((z + d) % hi, y, c), tp)) for d in range(1, hi)]
    y_copies = [forward(sp, y_send, y_recv, 0, to_y)]
    c_copies = [forward(sp, c_send, c_recv, 0, to_c)]

    add_in(last_block, last_slot, big, False)
    k_cols = ak.shape[1]
    halo[WINDOW : WINDOW + rows, 0:k_cols] = (ak[...] * scale).astype(BF16)
    halo[WINDOW : WINDOW + rows, k_cols : 2 * k_cols] = (av[...] * scale).astype(BF16)
    h_copies = [
        remote(halo.at[rows : rows + WINDOW], halo.at[0:WINDOW], h_send.at[0], h_recv.at[0], (right, tp)),
        remote(
            halo.at[WINDOW : 2 * WINDOW],
            halo.at[rows + WINDOW : rows + 2 * WINDOW],
            h_send.at[1],
            h_recv.at[1],
            (left, tp),
        ),
    ]
    for copy in h_copies:
        copy.start()
    qwin[...] = (aq[...] * scale).astype(BF16)
    per_head = UNROTATED_WIDTH + D_ROPE
    factor = per_head ** (-0.5) * LOG2E
    for h in range(alq.shape[1] // per_head):
        one = alq[:, h * per_head : (h + 1) * per_head] * scale
        plain = one[:, :UNROTATED_WIDTH].astype(BF16)
        seen = dot_nt(plain, kup_ref[:, h * UNROTATED_WIDTH : (h + 1) * UNROTATED_WIDTH]) * factor
        turned = turn(one[:, UNROTATED_WIDTH:], cosine, sine) * factor
        q_ref[h, :, 0:UNROTATED_WIDTH] = seen.astype(BF16)
        q_ref[h, :, UNROTATED_WIDTH:] = jnp.concatenate([turned, jnp.zeros_like(turned)], axis=1).astype(BF16)

    for d in range(1, hi):
        z_copies[d - 1].wait_recv()
        block = at((z + hi - d) % hi, y, c)
        y_copies.append(forward(block, y_send, y_recv, d, to_y))
        c_copies.append(forward(block, c_send, c_recv, d, to_c))
    for copy in h_copies:
        copy.wait()

    span = 3 * WINDOW
    spots = lax.broadcasted_iota(jnp.int32, (WINDOW, span), 0)
    keys_at = lax.broadcasted_iota(jnp.int32, (WINDOW, span), 1)
    distance = jnp.abs(spots + WINDOW - keys_at)
    far = distance.astype(F32)
    seq_total = rows * n_sp

    def window(kv_head):
        for b in range(rows // WINDOW):
            key_pos = sp * rows + (b - 1) * WINDOW + keys_at
            inside = (distance <= WINDOW) & (key_pos >= 0) & (key_pos < seq_total)
            keys = halo[b * WINDOW : b * WINDOW + span, kv_head * DH : (kv_head + 1) * DH]
            values = halo[b * WINDOW : b * WINDOW + span, k_cols + kv_head * DH : k_cols + (kv_head + 1) * DH]
            pieces = []
            for g in range(2):
                head = kv_head * 2 + g
                query = qwin[b * WINDOW : (b + 1) * WINDOW, head * DH : (head + 1) * DH]
                place = (tp * sink_ref.shape[0] + head + 1).astype(F32)
                slope = jnp.exp2(jnp.full((1, span), -8.0 / HEADS_A, F32) * place)
                scores = dot_nt(query, keys) * DH ** (-0.5) - slope * far
                scores = jnp.where(inside, scores, -jnp.inf)
                peak = jnp.maximum(jnp.max(scores, axis=1, keepdims=True), sink_ref[head])
                weight = jnp.exp(scores - peak)
                bottom = jnp.sum(weight, axis=1, keepdims=True) + jnp.exp(sink_ref[head] - peak)
                blended = jnp.dot(weight.astype(BF16), values, preferred_element_type=F32)
                pieces.append(blended / bottom)
            win_ref[b * WINDOW : (b + 1) * WINDOW, kv_head * 2 * DH : (kv_head + 1) * 2 * DH] = (
                jnp.concatenate(pieces, axis=1).astype(BF16)
            )

    kv_heads = k_cols // DH
    for kv_head in range((kv_heads + 1) // 2):
        window(kv_head)
    for d in range(hi):
        y_copies[d].wait_recv()
        c_copies.append(forward(at((z + hi - d) % hi, 1 - y, c), c_send, c_recv, hi + d, to_c))
    for kv_head in range((kv_heads + 1) // 2, kv_heads):
        window(kv_head)

    lanes = lax.broadcasted_iota(jnp.int32, (rows // 2, D_ROPE), 1)
    mark = jnp.where(lanes == 0, 1.0, 0.0).astype(BF16)

    def assemble(block):
        base = pl.multiple_of(block * rows, rows)
        kv_ref[pl.ds(base, rows), 0:UNROTATED_WIDTH] = gath[block, 0:rows, :]
        both = gath[block, rows : rows + rows // 2, :]
        kv_ref[pl.ds(base, rows // 2), UNROTATED_WIDTH:] = jnp.concatenate([both[:, :D_ROPE], mark], axis=1)
        kv_ref[pl.ds(base + rows // 2, rows // 2), UNROTATED_WIDTH:] = jnp.concatenate(
            [both[:, D_ROPE:], mark], axis=1
        )

    for d in range(hi):
        assemble(at((z + hi - d) % hi, y, c))
        assemble(at((z + hi - d) % hi, 1 - y, c))
    for d in range(hi):
        c_copies[d].wait_recv()
        assemble(at((z + hi - d) % hi, y, 1 - c))
    for d in range(hi):
        c_copies[hi + d].wait_recv()
        assemble(at((z + hi - d) % hi, 1 - y, 1 - c))
    for copy in list(x_copies.values()) + z_copies + y_copies + c_copies:
        copy.wait_send()


def attend_kernel(
    n_tp,
    q_ref, kv_ref, win_ref, vup_ref, ow_hbm, ol_hbm,
    out_ref,
    ow, ol, acc, peak, lat, outgoing, incoming, own, w_sem, send, recv,
):
    sp = lax.axis_index("sp")
    tp = lax.axis_index("tp")
    heads, rows, _ = q_ref.shape
    half = rows // 2
    cols = out_ref.shape[1]
    loads = [pltpu.make_async_copy(ow_hbm, ow, w_sem.at[0]), pltpu.make_async_copy(ol_hbm, ol, w_sem.at[1])]
    for load in loads:
        load.start()
    barrier = pltpu.get_barrier_semaphore()
    for s in range(1, n_tp):
        pl.semaphore_signal(barrier, inc=1, device_id=(sp, (tp + s) % n_tp), device_id_type=MESH)
    pl.semaphore_wait(barrier, n_tp - 1)

    chunk = min(1024, kv_ref.shape[0])
    copies = []
    for b in range(2):
        query = jnp.concatenate([q_ref[h, b * half : (b + 1) * half, :] for h in range(heads)], axis=0)
        acc[...] = jnp.zeros_like(acc)
        peak[...] = jnp.full_like(peak, -jnp.inf)

        def step(i, carry):
            keys = kv_ref[pl.ds(i * chunk if isinstance(i, int) else pl.multiple_of(i * chunk, chunk), chunk), :]
            scores = dot_nt(query, keys)
            old = peak[:, 0:1]
            new = jnp.maximum(old, jnp.max(scores, axis=1, keepdims=True))
            weight = jnp.exp2(scores - new).astype(BF16)
            acc[...] = acc[...] * jnp.exp2(old - new) + jnp.dot(weight, keys, preferred_element_type=F32)
            peak[...] = jnp.broadcast_to(new, peak.shape)
            return carry

        count = kv_ref.shape[0] // chunk
        if count > 4:
            lax.fori_loop(0, count, step, 0)
        else:
            for i in range(count):
                step(i, 0)
        bottom = acc[:, UNROTATED_WIDTH + D_ROPE : UNROTATED_WIDTH + D_ROPE + 1]
        blended = (acc[:, 0:VALUE_WIDTH] / bottom).astype(BF16)
        for h in range(heads):
            where = slice(h * VALUE_WIDTH, (h + 1) * VALUE_WIDTH)
            lat[:, where] = jnp.dot(
                blended[h * half : (h + 1) * half], vup_ref[:, where], preferred_element_type=F32
            ).astype(BF16)
        if b == 0:
            for load in loads:
                load.wait()
        won = win_ref[b * half : (b + 1) * half, :]

        def terms(j):
            where = pl.ds(pl.multiple_of(j * cols, cols), cols)
            return jnp.dot(won, ow[:, where], preferred_element_type=F32) + jnp.dot(
                lat[...], ol[:, where], preferred_element_type=F32
            )

        for s in range(1, n_tp):
            other = (tp + s) % n_tp
            outgoing[b, s - 1] = terms(other).astype(BF16)
            copy = pltpu.make_async_remote_copy(
                src_ref=outgoing.at[b, s - 1],
                dst_ref=incoming.at[b, s - 1],
                send_sem=send.at[b, s],
                recv_sem=recv.at[b, s],
                device_id=(sp, other),
                device_id_type=MESH,
            )
            copy.start()
            copies.append((b, s, copy))
        own[b] = terms(tp)
    for b in range(2):
        total = own[b]
        for bb, s, copy in copies:
            if bb == b:
                copy.wait()
                total = total + incoming[b, s - 1].astype(F32)
        out_ref[b * half : (b + 1) * half, :] = total.astype(BF16)


def per_device(
    n_sp, n_tp,
    activations, norm_gain, win_query, win_key, win_value, sink_logit, lat_query,
    key_value_down_weight, rope_key, latent_norm_gain, key_up_weight, value_up_weight, out_win, out_lat,
):
    rows, local = activations.shape
    width = local * n_tp
    part = local // SUB
    heads_a = sink_logit.shape[0]
    heads_l = lat_query.shape[1] // (UNROTATED_WIDTH + D_ROPE)
    frequency = 1.0 / ROPE_BASE ** (np.arange(0, D_ROPE, 2) / D_ROPE)
    frequency = np.concatenate([frequency, frequency])[None, :]
    near = np.arange(rows)[:, None] * frequency
    base = (np.arange(n_sp) * rows)[:, None] * frequency
    near = jnp.asarray(np.stack([np.cos(near), np.sin(near)]), F32)
    base = jnp.asarray(np.stack([np.cos(base), np.sin(base)], axis=1), F32)

    vmem = pl.BlockSpec(memory_space=pltpu.VMEM)
    smem = pl.BlockSpec(memory_space=pltpu.SMEM)
    hbm = pl.BlockSpec(memory_space=pl.ANY)
    weights = (key_value_down_weight, rope_key.T, win_key, win_value, win_query, lat_query)
    widths = [w.shape[0] if i == 1 else w.shape[1] for i, w in enumerate(weights)]
    hi = n_sp // 4
    dma = pltpu.SemaphoreType.DMA
    packed = rows + rows // 2
    query, keys, win_out = pl.pallas_call(
        functools.partial(project_kernel, n_sp, n_tp),
        out_shape=(
            jax.ShapeDtypeStruct((heads_l, rows, 2 * UNROTATED_WIDTH), BF16),
            jax.ShapeDtypeStruct((rows * n_sp, 2 * UNROTATED_WIDTH), BF16),
            jax.ShapeDtypeStruct((rows, heads_a * DH), BF16),
        ),
        in_specs=[vmem, vmem, vmem, vmem, smem, vmem, vmem] + [hbm] * 6,
        out_specs=(vmem, vmem, vmem),
        scratch_shapes=[pltpu.VMEM((n_tp * SUB, rows, part), BF16)]
        + [pltpu.VMEM(w.shape, BF16) for w in weights]
        + [pltpu.VMEM((rows, w), F32) for w in widths]
        + [
            pltpu.VMEM((rows, 128), F32),
            pltpu.VMEM((n_sp, packed, UNROTATED_WIDTH), BF16),
            pltpu.VMEM((rows + 2 * WINDOW, 2 * win_key.shape[1]), BF16),
            pltpu.VMEM((rows, win_query.shape[1]), BF16),
            dma((6,)),
            dma((n_tp, SUB)), dma((n_tp, SUB)),
            dma((hi,)), dma((hi,)),
            dma((hi,)), dma((hi,)),
            dma((2 * hi,)), dma((2 * hi,)),
            dma((2,)), dma((2,)),
        ],
        compiler_params=pltpu.CompilerParams(
            collective_id=0, has_side_effects=True, vmem_limit_bytes=56 * 1024 * 1024
        ),
        name="project",
    )(
        activations, norm_gain.reshape(n_tp * SUB, 1, part), near, base, sink_logit,
        latent_norm_gain.reshape(1, -1), key_up_weight, *weights,
    )
    return pl.pallas_call(
        functools.partial(attend_kernel, n_tp),
        out_shape=jax.ShapeDtypeStruct((rows, width // n_tp), BF16),
        in_specs=[vmem, vmem, vmem, vmem, hbm, hbm],
        out_specs=vmem,
        scratch_shapes=[
            pltpu.VMEM(out_win.shape, BF16),
            pltpu.VMEM(out_lat.shape, BF16),
            pltpu.VMEM((heads_l * rows // 2, 2 * UNROTATED_WIDTH), F32),
            pltpu.VMEM((heads_l * rows // 2, 128), F32),
            pltpu.VMEM((rows // 2, heads_l * VALUE_WIDTH), BF16),
            pltpu.VMEM((2, n_tp - 1, rows // 2, width // n_tp), BF16),
            pltpu.VMEM((2, n_tp - 1, rows // 2, width // n_tp), BF16),
            pltpu.VMEM((2, rows // 2, width // n_tp), F32),
            dma((2,)),
            dma((2, n_tp)), dma((2, n_tp)),
        ],
        compiler_params=pltpu.CompilerParams(
            collective_id=1, has_side_effects=True, vmem_limit_bytes=56 * 1024 * 1024
        ),
        name="attend",
    )(query, keys, win_out, value_up_weight, out_win, out_lat)


def solution(mesh):
    return jax.shard_map(
        functools.partial(per_device, mesh.shape["sp"], mesh.shape["tp"]),
        mesh=mesh,
        in_specs=(
            P("sp", "tp"),
            P(),
            P(None, "tp"),
            P(None, "tp"),
            P(None, "tp"),
            P("tp"),
            P(None, "tp"),
            P(),
            P(),
            P(),
            P(None, "tp"),
            P(None, "tp"),
            P("tp", None),
            P("tp", None),
        ),
        out_specs=P("sp", "tp"),
        check_vma=False,
    )
```

```python
import functools

import jax
import jax.numpy as jnp
import numpy as np
from jax import lax
from jax.experimental import pallas as pl
from jax.experimental.pallas import tpu as pltpu
from jax.sharding import PartitionSpec as P

HEADS_A = 16
DH = 64
WINDOW = 128
UNROTATED_WIDTH = 128
D_ROPE = 64
VALUE_WIDTH = 128

EPSILON = 1e-06
ROPE_BASE = 10000.0
LOG2E = 1.4426950408889634
MESH = pl.DeviceIdType.MESH
F32 = jnp.float32
BF16 = jnp.bfloat16
SUB = 2
BANDS = 4


def turn(vectors, cosine, sine):
    half = vectors.shape[-1] // 2
    swapped = jnp.concatenate([vectors[:, half:], vectors[:, :half]], axis=1)
    return vectors * cosine + swapped * sine


def dot_nt(a, b):
    return lax.dot_general(a, b, (((1,), (1,)), ((), ())), preferred_element_type=F32)


def project_kernel(
    n_sp, n_tp,
    x_ref, gain_ref, near_ref, base_ref, sink_ref, lng_ref, kup_ref,
    wkv_hbm, wr_hbm, wk_hbm, wv_hbm, wq_hbm, wlq_hbm,
    q_ref, kv_ref, win_ref,
    x_all, wkv, wr, wk, wv, wq, wlq, akv, ar, ak, av, aq, alq, sq, gath, halo, qwin,
    w_sem, x_send, x_recv, z_send, z_recv, y_send, y_recv, c_send, c_recv, h_send, h_recv,
):
    sp = lax.axis_index("sp")
    tp = lax.axis_index("tp")
    rows, local = x_ref.shape
    part = local // SUB
    hi = n_sp // 4
    z, y, c = sp // 4, (sp // 2) % 2, sp % 2

    def at(zz, yy, cc):
        return (zz * 2 + yy) * 2 + cc

    right, left = (sp + 1) % n_sp, (sp + n_sp - 1) % n_sp

    weights = ((wkv_hbm, wkv), (wr_hbm, wr), (wk_hbm, wk), (wv_hbm, wv), (wq_hbm, wq), (wlq_hbm, wlq))
    loads = [pltpu.make_async_copy(a, b, w_sem.at[i]) for i, (a, b) in enumerate(weights)]
    for load in loads:
        load.start()

    barrier = pltpu.get_barrier_semaphore()
    peers = [(sp, (tp + s) % n_tp) for s in range(1, n_tp)]
    peers += [(at((z + d) % hi, y, c), tp) for d in range(1, hi)]
    peers += [(at(z, 1 - y, c), tp), (at(z, y, 1 - c), tp), (right, tp), (left, tp)]
    for peer in peers:
        pl.semaphore_signal(barrier, inc=1, device_id=peer, device_id_type=MESH)
    pl.semaphore_wait(barrier, len(peers))

    def remote(src, dst, send, recv, device):
        return pltpu.make_async_remote_copy(
            src_ref=src, dst_ref=dst, send_sem=send, recv_sem=recv, device_id=device, device_id_type=MESH
        )

    x_copies = {}
    for cc in range(SUB):
        for s in range(1, n_tp):
            x_copies[s, cc] = remote(
                x_ref.at[:, cc * part : (cc + 1) * part],
                x_all.at[tp * SUB + cc],
                x_send.at[s, cc],
                x_recv.at[s, cc],
                (sp, (tp + s) % n_tp),
            )
            x_copies[s, cc].start()

    def add_in(block, slot, pairs, first):
        where = pl.ds(pl.multiple_of(slot * part, part), part)
        for weight, acc in pairs:
            if weight is wr:
                term = dot_nt(block, weight[:, where])
            else:
                term = jnp.dot(block, weight[where, :], preferred_element_type=F32)
            acc[...] = term if first else acc[...] + term

    def norm_block(raw, slot, first):
        wide = raw.astype(F32)
        total = jnp.broadcast_to(jnp.sum(wide * wide, axis=1, keepdims=True), sq.shape)
        sq[...] = total if first else sq[...] + total
        return (wide * gain_ref[slot]).astype(BF16)

    near_cos, near_sin = near_ref[0], near_ref[1]
    base_cos, base_sin = base_ref[sp, 0:1, :], base_ref[sp, 1:2, :]
    cosine = near_cos * base_cos - near_sin * base_sin
    plain_sine = near_sin * base_cos + near_cos * base_sin
    lane = lax.broadcasted_iota(jnp.int32, plain_sine.shape, 1)
    sine = jnp.where(lane < D_ROPE // 2, -plain_sine, plain_sine)
    small = ((wkv, akv), (wr, ar))
    big = ((wk, ak), (wv, av), (wq, aq), (wlq, alq))
    for load in loads:
        load.wait()
    for cc in range(SUB):
        slot = tp * SUB + cc
        block = norm_block(x_ref[:, cc * part : (cc + 1) * part], slot, cc == 0)
        add_in(block, slot, small + big, cc == 0)
    steps = [(s, cc) for cc in range(SUB) for s in range(1, n_tp)]
    for s, cc in steps[:-1]:
        x_copies[s, cc].wait_recv()
        slot = ((tp + n_tp - s) % n_tp) * SUB + cc
        add_in(norm_block(x_all[slot], slot, False), slot, small + big, False)
    s, cc = steps[-1]
    x_copies[s, cc].wait_recv()
    last_slot = ((tp + n_tp - s) % n_tp) * SUB + cc
    last_block = norm_block(x_all[last_slot], last_slot, False)
    add_in(last_block, last_slot, small, False)

    scale = lax.rsqrt(sq[:, 0:1] / (local * n_tp) + EPSILON)
    comp = akv[...]
    latent = comp * lax.rsqrt(jnp.mean(comp * comp, axis=1, keepdims=True) + EPSILON) * lng_ref[...]
    rotary = turn(ar[...] * scale, cosine, sine)
    gath[sp, 0:rows, :] = latent.astype(BF16)
    gath[sp, rows : rows + rows // 2, :] = jnp.concatenate(
        [rotary[: rows // 2], rotary[rows // 2 :]], axis=1
    ).astype(BF16)

    def forward(block, sends, recvs, index, device):
        copy = remote(gath.at[block], gath.at[block], sends.at[index], recvs.at[index], device)
        copy.start()
        return copy

    to_y, to_c = (at(z, 1 - y, c), tp), (at(z, y, 1 - c), tp)
    z_copies = [forward(sp, z_send, z_recv, d, (at((z + d) % hi, y, c), tp)) for d in range(1, hi)]
    y_copies = [forward(sp, y_send, y_recv, 0, to_y)]
    c_copies = [forward(sp, c_send, c_recv, 0, to_c)]

    add_in(last_block, last_slot, big, False)
    k_cols = ak.shape[1]
    halo[WINDOW : WINDOW + rows, 0:k_cols] = (ak[...] * scale).astype(BF16)
    halo[WINDOW : WINDOW + rows, k_cols : 2 * k_cols] = (av[...] * scale).astype(BF16)
    h_copies = [
        remote(halo.at[rows : rows + WINDOW], halo.at[0:WINDOW], h_send.at[0], h_recv.at[0], (right, tp)),
        remote(
            halo.at[WINDOW : 2 * WINDOW],
            halo.at[rows + WINDOW : rows + 2 * WINDOW],
            h_send.at[1],
            h_recv.at[1],
            (left, tp),
        ),
    ]
    for copy in h_copies:
        copy.start()
    qwin[...] = (aq[...] * scale).astype(BF16)
    per_head = UNROTATED_WIDTH + D_ROPE
    factor = per_head ** (-0.5) * LOG2E
    for h in range(alq.shape[1] // per_head):
        one = alq[:, h * per_head : (h + 1) * per_head] * scale
        plain = one[:, :UNROTATED_WIDTH].astype(BF16)
        seen = dot_nt(plain, kup_ref[:, h * UNROTATED_WIDTH : (h + 1) * UNROTATED_WIDTH]) * factor
        turned = turn(one[:, UNROTATED_WIDTH:], cosine, sine) * factor
        q_ref[h, :, 0:UNROTATED_WIDTH] = seen.astype(BF16)
        q_ref[h, :, UNROTATED_WIDTH:] = jnp.concatenate([turned, jnp.zeros_like(turned)], axis=1).astype(BF16)

    for d in range(1, hi):
        z_copies[d - 1].wait_recv()
        block = at((z + hi - d) % hi, y, c)
        y_copies.append(forward(block, y_send, y_recv, d, to_y))
        c_copies.append(forward(block, c_send, c_recv, d, to_c))
    for copy in h_copies:
        copy.wait()

    span = 3 * WINDOW
    spots = lax.broadcasted_iota(jnp.int32, (WINDOW, span), 0)
    keys_at = lax.broadcasted_iota(jnp.int32, (WINDOW, span), 1)
    distance = jnp.abs(spots + WINDOW - keys_at)
    far = distance.astype(F32)
    seq_total = rows * n_sp

    def window(kv_head):
        for b in range(rows // WINDOW):
            key_pos = sp * rows + (b - 1) * WINDOW + keys_at
            inside = (distance <= WINDOW) & (key_pos >= 0) & (key_pos < seq_total)
            keys = halo[b * WINDOW : b * WINDOW + span, kv_head * DH : (kv_head + 1) * DH]
            values = halo[b * WINDOW : b * WINDOW + span, k_cols + kv_head * DH : k_cols + (kv_head + 1) * DH]
            pieces = []
            for g in range(2):
                head = kv_head * 2 + g
                query = qwin[b * WINDOW : (b + 1) * WINDOW, head * DH : (head + 1) * DH]
                place = (tp * sink_ref.shape[0] + head + 1).astype(F32)
                slope = jnp.exp2(jnp.full((1, span), -8.0 / HEADS_A, F32) * place)
                scores = dot_nt(query, keys) * DH ** (-0.5) - slope * far
                scores = jnp.where(inside, scores, -jnp.inf)
                peak = jnp.maximum(jnp.max(scores, axis=1, keepdims=True), sink_ref[head])
                weight = jnp.exp(scores - peak)
                bottom = jnp.sum(weight, axis=1, keepdims=True) + jnp.exp(sink_ref[head] - peak)
                blended = jnp.dot(weight.astype(BF16), values, preferred_element_type=F32)
                pieces.append(blended / bottom)
            win_ref[b * WINDOW : (b + 1) * WINDOW, kv_head * 2 * DH : (kv_head + 1) * 2 * DH] = (
                jnp.concatenate(pieces, axis=1).astype(BF16)
            )

    kv_heads = k_cols // DH
    for kv_head in range((kv_heads + 1) // 2):
        window(kv_head)
    for d in range(hi):
        y_copies[d].wait_recv()
        c_copies.append(forward(at((z + hi - d) % hi, 1 - y, c), c_send, c_recv, hi + d, to_c))
    for kv_head in range((kv_heads + 1) // 2, kv_heads):
        window(kv_head)

    lanes = lax.broadcasted_iota(jnp.int32, (rows // 2, D_ROPE), 1)
    mark = jnp.where(lanes == 0, 1.0, 0.0).astype(BF16)

    def assemble(block):
        base = pl.multiple_of(block * rows, rows)
        kv_ref[pl.ds(base, rows), 0:UNROTATED_WIDTH] = gath[block, 0:rows, :]
        both = gath[block, rows : rows + rows // 2, :]
        kv_ref[pl.ds(base, rows // 2), UNROTATED_WIDTH:] = jnp.concatenate([both[:, :D_ROPE], mark], axis=1)
        kv_ref[pl.ds(base + rows // 2, rows // 2), UNROTATED_WIDTH:] = jnp.concatenate(
            [both[:, D_ROPE:], mark], axis=1
        )

    for d in range(hi):
        assemble(at((z + hi - d) % hi, y, c))
        assemble(at((z + hi - d) % hi, 1 - y, c))
    for d in range(hi):
        c_copies[d].wait_recv()
        assemble(at((z + hi - d) % hi, y, 1 - c))
    for d in range(hi):
        c_copies[hi + d].wait_recv()
        assemble(at((z + hi - d) % hi, 1 - y, 1 - c))
    for copy in list(x_copies.values()) + z_copies + y_copies + c_copies:
        copy.wait_send()


def attend_kernel(
    n_tp,
    q_ref, kv_ref, win_ref, vup_ref, ow_hbm, ol_hbm,
    out_ref,
    ow, ol, acc, peak, lat, outgoing, incoming, own, w_sem, send, recv,
):
    sp = lax.axis_index("sp")
    tp = lax.axis_index("tp")
    heads, rows, _ = q_ref.shape
    half = rows // BANDS
    cols = out_ref.shape[1]
    loads = [pltpu.make_async_copy(ow_hbm, ow, w_sem.at[0]), pltpu.make_async_copy(ol_hbm, ol, w_sem.at[1])]
    for load in loads:
        load.start()
    barrier = pltpu.get_barrier_semaphore()
    for s in range(1, n_tp):
        pl.semaphore_signal(barrier, inc=1, device_id=(sp, (tp + s) % n_tp), device_id_type=MESH)
    pl.semaphore_wait(barrier, n_tp - 1)

    chunk = min(1024, kv_ref.shape[0])
    copies = []
    for b in range(BANDS):
        query = jnp.concatenate([q_ref[h, b * half : (b + 1) * half, :] for h in range(heads)], axis=0)
        acc[...] = jnp.zeros_like(acc)
        peak[...] = jnp.full_like(peak, -jnp.inf)

        def step(i, carry):
            keys = kv_ref[pl.ds(i * chunk if isinstance(i, int) else pl.multiple_of(i * chunk, chunk), chunk), :]
            scores = dot_nt(query, keys)
            old = peak[:, 0:1]
            new = jnp.maximum(old, jnp.max(scores, axis=1, keepdims=True))
            weight = jnp.exp2(scores - new).astype(BF16)
            acc[...] = acc[...] * jnp.exp2(old - new) + jnp.dot(weight, keys, preferred_element_type=F32)
            peak[...] = jnp.broadcast_to(new, peak.shape)
            return carry

        count = kv_ref.shape[0] // chunk
        if count > 4:
            lax.fori_loop(0, count, step, 0)
        else:
            for i in range(count):
                step(i, 0)
        bottom = acc[:, UNROTATED_WIDTH + D_ROPE : UNROTATED_WIDTH + D_ROPE + 1]
        blended = (acc[:, 0:VALUE_WIDTH] / bottom).astype(BF16)
        for h in range(heads):
            where = slice(h * VALUE_WIDTH, (h + 1) * VALUE_WIDTH)
            lat[:, where] = jnp.dot(
                blended[h * half : (h + 1) * half], vup_ref[:, where], preferred_element_type=F32
            ).astype(BF16)
        if b == 0:
            for load in loads:
                load.wait()
        won = win_ref[b * half : (b + 1) * half, :]

        def terms(j):
            where = pl.ds(pl.multiple_of(j * cols, cols), cols)
            return jnp.dot(won, ow[:, where], preferred_element_type=F32) + jnp.dot(
                lat[...], ol[:, where], preferred_element_type=F32
            )

        for s in range(1, n_tp):
            other = (tp + s) % n_tp
            outgoing[b, s - 1] = terms(other).astype(BF16)
            copy = pltpu.make_async_remote_copy(
                src_ref=outgoing.at[b, s - 1],
                dst_ref=incoming.at[b, s - 1],
                send_sem=send.at[b, s],
                recv_sem=recv.at[b, s],
                device_id=(sp, other),
                device_id_type=MESH,
            )
            copy.start()
            copies.append((b, s, copy))
        own[b] = terms(tp)
    for b in range(BANDS):
        total = own[b]
        for bb, s, copy in copies:
            if bb == b:
                copy.wait()
                total = total + incoming[b, s - 1].astype(F32)
        out_ref[b * half : (b + 1) * half, :] = total.astype(BF16)


def per_device(
    n_sp, n_tp,
    activations, norm_gain, win_query, win_key, win_value, sink_logit, lat_query,
    key_value_down_weight, rope_key, latent_norm_gain, key_up_weight, value_up_weight, out_win, out_lat,
):
    rows, local = activations.shape
    width = local * n_tp
    part = local // SUB
    heads_a = sink_logit.shape[0]
    heads_l = lat_query.shape[1] // (UNROTATED_WIDTH + D_ROPE)
    frequency = 1.0 / ROPE_BASE ** (np.arange(0, D_ROPE, 2) / D_ROPE)
    frequency = np.concatenate([frequency, frequency])[None, :]
    near = np.arange(rows)[:, None] * frequency
    base = (np.arange(n_sp) * rows)[:, None] * frequency
    near = jnp.asarray(np.stack([np.cos(near), np.sin(near)]), F32)
    base = jnp.asarray(np.stack([np.cos(base), np.sin(base)], axis=1), F32)

    vmem = pl.BlockSpec(memory_space=pltpu.VMEM)
    smem = pl.BlockSpec(memory_space=pltpu.SMEM)
    hbm = pl.BlockSpec(memory_space=pl.ANY)
    weights = (key_value_down_weight, rope_key.T, win_key, win_value, win_query, lat_query)
    widths = [w.shape[0] if i == 1 else w.shape[1] for i, w in enumerate(weights)]
    hi = n_sp // 4
    dma = pltpu.SemaphoreType.DMA
    packed = rows + rows // 2
    query, keys, win_out = pl.pallas_call(
        functools.partial(project_kernel, n_sp, n_tp),
        out_shape=(
            jax.ShapeDtypeStruct((heads_l, rows, 2 * UNROTATED_WIDTH), BF16),
            jax.ShapeDtypeStruct((rows * n_sp, 2 * UNROTATED_WIDTH), BF16),
            jax.ShapeDtypeStruct((rows, heads_a * DH), BF16),
        ),
        in_specs=[vmem, vmem, vmem, vmem, smem, vmem, vmem] + [hbm] * 6,
        out_specs=(vmem, vmem, vmem),
        scratch_shapes=[pltpu.VMEM((n_tp * SUB, rows, part), BF16)]
        + [pltpu.VMEM(w.shape, BF16) for w in weights]
        + [pltpu.VMEM((rows, w), F32) for w in widths]
        + [
            pltpu.VMEM((rows, 128), F32),
            pltpu.VMEM((n_sp, packed, UNROTATED_WIDTH), BF16),
            pltpu.VMEM((rows + 2 * WINDOW, 2 * win_key.shape[1]), BF16),
            pltpu.VMEM((rows, win_query.shape[1]), BF16),
            dma((6,)),
            dma((n_tp, SUB)), dma((n_tp, SUB)),
            dma((hi,)), dma((hi,)),
            dma((hi,)), dma((hi,)),
            dma((2 * hi,)), dma((2 * hi,)),
            dma((2,)), dma((2,)),
        ],
        compiler_params=pltpu.CompilerParams(
            collective_id=0, has_side_effects=True, vmem_limit_bytes=56 * 1024 * 1024
        ),
        name="project",
    )(
        activations, norm_gain.reshape(n_tp * SUB, 1, part), near, base, sink_logit,
        latent_norm_gain.reshape(1, -1), key_up_weight, *weights,
    )
    return pl.pallas_call(
        functools.partial(attend_kernel, n_tp),
        out_shape=jax.ShapeDtypeStruct((rows, width // n_tp), BF16),
        in_specs=[vmem, vmem, vmem, vmem, hbm, hbm],
        out_specs=vmem,
        scratch_shapes=[
            pltpu.VMEM(out_win.shape, BF16),
            pltpu.VMEM(out_lat.shape, BF16),
            pltpu.VMEM((heads_l * rows // BANDS, 2 * UNROTATED_WIDTH), F32),
            pltpu.VMEM((heads_l * rows // BANDS, 128), F32),
            pltpu.VMEM((rows // BANDS, heads_l * VALUE_WIDTH), BF16),
            pltpu.VMEM((BANDS, n_tp - 1, rows // BANDS, width // n_tp), BF16),
            pltpu.VMEM((BANDS, n_tp - 1, rows // BANDS, width // n_tp), BF16),
            pltpu.VMEM((BANDS, rows // BANDS, width // n_tp), F32),
            dma((2,)),
            dma((BANDS, n_tp)), dma((BANDS, n_tp)),
        ],
        compiler_params=pltpu.CompilerParams(
            collective_id=1, has_side_effects=True, vmem_limit_bytes=56 * 1024 * 1024
        ),
        name="attend",
    )(query, keys, win_out, value_up_weight, out_win, out_lat)


def solution(mesh):
    return jax.shard_map(
        functools.partial(per_device, mesh.shape["sp"], mesh.shape["tp"]),
        mesh=mesh,
        in_specs=(
            P("sp", "tp"),
            P(),
            P(None, "tp"),
            P(None, "tp"),
            P(None, "tp"),
            P("tp"),
            P(None, "tp"),
            P(),
            P(),
            P(),
            P(None, "tp"),
            P(None, "tp"),
            P("tp", None),
            P("tp", None),
        ),
        out_specs=P("sp", "tp"),
        check_vma=False,
    )
```
